32 devices in a mesh: ep: 8 (over z, core), tp: 4 (over y, x).
Axes of the slice: x: 2, y: 2, z: 4, core: 2. Of those that a mesh axis runs over, the one named last changes fastest.
Arguments:
- pool_input: bfloat16 [2048, 2048], P('ep'), may hold values from -6 to 6
- pool_gain: float32 [2048], replicated, may hold values from 0.1 to 1.9
- pool_weight: bfloat16 [512, 2048], P(None, 'tp'), may hold values from -0.25 to 0.25
- pool_scale: float32 [2048], P('tp'), may hold values from 0.1 to 1.9
- moe_input: bfloat16 [1536, 2048], P('ep'), may hold values from -6 to 6
- moe_gain: float32 [2048], replicated, may hold values from 0.1 to 1.9
- routes: int32 [1536, 2], P('ep'), may hold values from 0 to 7, all different within a row; in each aligned block of 192 rows (0 to 191, 192 to 383, ...) at most 96 rows name the same one
- route_logits: float32 [1536, 2], P('ep'), may hold values from -4 to 4
- gate_weight: bfloat16 [8, 2048, 4096], P('ep', None, 'tp'), may hold values from -0.125 to 0.125
- up_weight: bfloat16 [8, 2048, 4096], P('ep', None, 'tp'), may hold values from -0.125 to 0.125
- down_weight: bfloat16 [8, 2048, 4096], P('ep', None, 'tp'), may hold values from -0.09375 to 0.09375
Outputs:
- pool_out: bfloat16 [2048, 2048], P('ep', 'tp')
- expert_out: bfloat16 [1536, 2048], P('ep', 'tp')
The draws below stay inside these ranges and needn't reach their ends.
Inputs may be any that keep to these rules, and one draw needn't show every extreme that they name: `routes`: the 2 experts of a token differ. Within the rows of one device (aligned blocks of 192 rows) no expert is named by more than 96 rows, and in every draw some expert is named by exactly 96 rows of some device.
All inputs are finite; a program needn't handle non-finite values.
Results may differ from the reference program's by a relative error of at most 0.017.
Values may be sent and summed in bfloat16 or wider, within the bound.
A program may use at most 64 MiB of HBM per device.

```python
import math
from functools import partial
import jax
import jax.numpy as jnp
import numpy as np
from jax import lax

D = 2048
GROUP_WIDTH = 512
FE = 4096
TOPK = 2
TOK_B = 192
EXPERTS = 8
CAPACITY = 96
TOKENS_A = 2048
TOKENS_B = 1536
N_EP = 8
N_TP = 4


def block_scale(rng, dims, shards, low, high):
    gain = 1.0
    for axis_at, blocks in shards:
        draws = jax.random.uniform(jax.random.fold_in(jax.random.fold_in(rng, 6), axis_at), (blocks,), jnp.float32, low / len(shards), high / len(shards))
        gain = gain * jnp.repeat(jnp.exp(draws), dims[axis_at] // blocks).reshape((-1,) + (1,) * (len(dims) - 1 - axis_at))
    return gain


def assign_block(own_key, own, number, rows, amount, top, bound, slope):
    order = jax.random.permutation(own_key, amount)
    heavy_load, usual = portions_of(amount, rows * top, bound, slope, True), portions_of(amount, rows * top, bound, slope, False)
    places = jnp.arange(amount)

    def named(lengths, turn):
        used = int((lengths > 0).sum())
        fixed = max(1, used // 4)
        passed = fixed + (places - fixed + turn * (used - fixed)) % max(1, amount - fixed)
        return jnp.zeros((amount,), jnp.int32).at[order[jnp.where(places < fixed, places, passed)]].set(jnp.asarray(lengths, jnp.int32))

    lengths = jnp.where(number % 4 == 0, named(heavy_load, number // 4), named(usual, number - number // 4 - 1))
    mixed = jax.random.permutation(jax.random.fold_in(own, 3), amount)
    source_of, receiver = mixed[0:amount // 2 * 2:2], mixed[1:amount // 2 * 2:2]
    slack = jnp.minimum(lengths[source_of] - 1, bound - lengths[receiver]) // 2
    slack = jnp.where((source_of == order[0]) | (receiver == order[0]) | (lengths[receiver] == 0), 0, jnp.maximum(slack, 0))
    passed = jax.random.randint(jax.random.fold_in(own, 4), (amount // 2,), 0, 1 << 20) % (slack + 1)
    lengths = lengths.at[source_of].add(-passed).at[receiver].add(passed)
    members = jnp.searchsorted(jnp.cumsum(lengths), jnp.arange(rows * top), side="right").astype(jnp.int32)
    listing = members.reshape(top, rows).T
    listing = listing[jax.random.permutation(jax.random.fold_in(own, 1), rows)]
    turn = jax.random.randint(jax.random.fold_in(own, 2), (rows, 1), 0, top)
    return jnp.take_along_axis(listing, (jnp.arange(top)[None, :] + turn) % top, axis=1)


def portions_of(amount, total, bound, lean, full):
    loads = [(1 << 20) // math.isqrt(grade ** lean) + 1 for grade in range(1, amount + 1)]
    largest = bound if full else min(bound, max(-(-total // amount), total * loads[0] // sum(loads)))
    least = 1 if total - largest >= amount - 1 else 0
    holding, spare = [largest] + [least] * (amount - 1), total - largest - least * (amount - 1)
    while spare > 0:
        candidates = [i for i in range(1, amount) if holding[i] < largest] or [i for i in range(1, amount) if holding[i] < bound]
        whole, remaining = sum([loads[i] for i in candidates]), spare
        for i in candidates:
            more = min(bound - holding[i], max(1, remaining * loads[i] // whole), spare)
            holding[i] = holding[i] + more
            spare = spare - more
    return np.array(holding)


def gaussian(rng, shape, scale, limit, split=(), kind=jnp.bfloat16):
    drawn = scale * jax.random.normal(rng, shape, jnp.float32)
    if split:
        drawn = drawn * block_scale(rng, shape, split, -0.22, 0.18)
    return jnp.clip(drawn, -limit, limit).astype(kind)


def setup_inputs(seed: int = 0) -> dict:
    arg_keys = jax.random.split(jax.random.key(seed), 12)
    pool_input = gaussian(arg_keys[0], (TOKENS_A, D), 1.0, 6.0, ((0, 8),))
    pool_gain = jnp.clip(1.0 + 0.18 * jax.random.normal(arg_keys[1], (D,), jnp.float32), 0.1, 1.9)
    pool_weight = gaussian(arg_keys[2], (GROUP_WIDTH, D), GROUP_WIDTH ** -0.5, 0.25, ((1, 4),))
    pool_scale = jnp.clip(1.0 + 0.18 * jax.random.normal(arg_keys[3], (D,), jnp.float32), 0.1, 1.9)
    moe_input = gaussian(arg_keys[4], (TOKENS_B, D), 1.0, 6.0, ((0, 8),))
    moe_gain = jnp.clip(1.0 + 0.18 * jax.random.normal(arg_keys[5], (D,), jnp.float32), 0.1, 1.9)
    routes_keys = jax.random.split(jax.random.fold_in(arg_keys[6], 1), TOKENS_B // TOK_B)
    routes_turns = jax.random.permutation(jax.random.fold_in(arg_keys[6], 3), TOKENS_B // TOK_B)
    routes = jax.vmap(lambda own, number: assign_block(jax.random.fold_in(arg_keys[6], 2), own, number, TOK_B, EXPERTS, TOPK, CAPACITY, 2))(routes_keys, routes_turns).reshape((TOKENS_B, TOPK))
    route_logits = gaussian(arg_keys[7], (TOKENS_B, TOPK), 1.0, 4.0, ((0, 8),), jnp.float32)
    gate_weight = gaussian(arg_keys[8], (EXPERTS, D, FE), D ** -0.5, 0.125, ((0, 8), (2, 4)))
    up_weight = gaussian(arg_keys[9], (EXPERTS, D, FE), D ** -0.5, 0.125, ((0, 8), (2, 4)))
    down_weight = gaussian(arg_keys[10], (EXPERTS, D, FE), FE ** -0.5, 0.09375, ((0, 8), (2, 4)))
    return {"pool_input": pool_input, "pool_gain": pool_gain, "pool_weight": pool_weight, "pool_scale": pool_scale, "moe_input": moe_input, "moe_gain": moe_gain, "routes": routes, "route_logits": route_logits, "gate_weight": gate_weight, "up_weight": up_weight, "down_weight": down_weight}


EPSILON = 1e-06

def rms_rows(row_block, scale_gain):
    values = row_block.astype(jnp.float32)
    scaled = values * lax.rsqrt(lax.optimization_barrier(jnp.mean(values * values, axis=-1, keepdims=True)) + EPSILON)
    return (scaled * scale_gain).astype(jnp.bfloat16)

def delayed(values, offset):
    return jnp.concatenate([jnp.zeros((offset,) + values.shape[1:], values.dtype), values[:-offset]], axis=0)

def window_sums(values):
    totals = []
    current = values
    for offset in (1, 2, 4, 8):
        current = current + delayed(current, offset)
        totals.append(current)
    return totals

def slot_tables(route_block, expert_count, capacity):
    tokens_count = route_block.shape[0]
    picks_count = route_block.shape[1]
    flat_ids = route_block.reshape(-1)
    onehot = (flat_ids[:, None] == jnp.arange(expert_count, dtype=jnp.int32)[None, :]).astype(jnp.int32)
    before = jnp.cumsum(onehot, axis=0) - onehot
    rank_in = lax.optimization_barrier(jnp.sum(before * onehot, axis=1))
    slot_ids = (flat_ids * capacity + rank_in).astype(jnp.int32)
    owners = jnp.repeat(jnp.arange(tokens_count, dtype=jnp.int32), picks_count)
    holder = jnp.full((expert_count * capacity,), tokens_count, jnp.int32).at[slot_ids].set(owners)
    return (slot_ids, holder)

def pick_rows(source, indices):
    return source[indices]

def reference(pool_input, pool_gain, pool_weight, pool_scale, moe_input, moe_gain, routes, route_logits, gate_weight, up_weight, down_weight):
    normed = rms_rows(pool_input, pool_gain)
    values = normed.astype(jnp.float32)
    sums_all = window_sums(values)
    position = jnp.arange(normed.shape[0], dtype=jnp.int32)
    pieces = []
    for group_index in range(4):
        window = 2 << group_index
        first_col = group_index * GROUP_WIDTH
        counts = jnp.minimum(position + 1, window).astype(jnp.float32)
        pooled = sums_all[group_index][:, first_col:first_col + GROUP_WIDTH] / counts[:, None]
        mixed_in = (pooled - values[:, first_col:first_col + GROUP_WIDTH]).astype(jnp.bfloat16)
        pieces.append(jnp.dot(mixed_in, pool_weight[:, first_col:first_col + GROUP_WIDTH], preferred_element_type=jnp.float32))
    pool_out = (jnp.concatenate(pieces, axis=1) * pool_scale).astype(jnp.bfloat16)
    normed_b = rms_rows(moe_input, moe_gain)
    blocks = normed_b.reshape(N_EP, TOK_B, D)
    route_blocks = routes.reshape(N_EP, TOK_B, TOPK)
    slot_ids, holder = jax.vmap(partial(slot_tables, expert_count=EXPERTS, capacity=CAPACITY))(route_blocks)
    padded = jnp.concatenate([blocks, jnp.zeros((N_EP, 1, D), jnp.bfloat16)], axis=1)
    gathered = jax.vmap(pick_rows)(padded, holder)
    per_expert = gathered.reshape(N_EP, EXPERTS, CAPACITY, D).transpose(1, 0, 2, 3).reshape(EXPERTS, N_EP * CAPACITY, D)

    def run_expert(operands):
        rows_in, gate_block, up_block, down_block = operands
        rows_wide = rows_in.astype(jnp.float32)
        gate_part = jnp.dot(rows_wide, gate_block.astype(jnp.float32), preferred_element_type=jnp.float32)
        up_part = jnp.dot(rows_wide, up_block.astype(jnp.float32), preferred_element_type=jnp.float32)
        hidden = (jax.nn.silu(gate_part) * up_part).astype(jnp.bfloat16)
        share_width = FE // N_TP
        hidden_shares = hidden.reshape(rows_in.shape[0], N_TP, share_width).astype(jnp.float32)
        down_shares = down_block.reshape(D, N_TP, share_width).astype(jnp.float32)
        partial_sums = jnp.einsum('rsf,dsf->srd', hidden_shares, down_shares).astype(jnp.bfloat16)
        return lax.optimization_barrier(jnp.sum(partial_sums.astype(jnp.float32), axis=0)).astype(jnp.bfloat16)
    outputs = lax.map(run_expert, (per_expert, gate_weight, up_weight, down_weight))
    expert_ids = route_blocks.reshape(N_EP, TOK_B * TOPK)
    rank_in = slot_ids - expert_ids * CAPACITY
    block_ids = jnp.arange(N_EP, dtype=jnp.int32)[:, None]
    global_index = (expert_ids * (N_EP * CAPACITY) + block_ids * CAPACITY + rank_in).astype(jnp.int32)
    flat_out = outputs.reshape(EXPERTS * N_EP * CAPACITY, D)[global_index.reshape(-1)]
    picked = flat_out.reshape(N_EP * TOK_B, TOPK, D).astype(jnp.float32)
    raised = jnp.exp(route_logits)
    weights = raised / lax.optimization_barrier(jnp.sum(raised, axis=-1, keepdims=True))
    combined = jnp.einsum('tkd,tk->td', picked, weights)
    return (pool_out, combined.astype(jnp.bfloat16))
```

```python
import functools

import jax
import jax.numpy as jnp
from jax import lax
from jax.experimental import pallas as pl
from jax.experimental.pallas import tpu as pltpu
from jax.sharding import PartitionSpec as P

EPSILON = 1e-06
halo_rows = 16


def plane_orders(planes):
    if planes == 4:
        return [[1, 3, 2], [0, 2, 3], [3, 1, 0], [2, 0, 1]]
    return [[(p + step) % planes for step in range(1, planes)] for p in range(planes)]


FOUR_PLANES = (
    "ZS10", "ZS20", "PS00", "ZS30", "SF11", "OWN00", "SF10", "ZD10", "GU01", "SF21", "GU00",
    "SF20", "DN00", "SP00", "SS21", "SS20", "SF31", "ZD30", "SF30", "SE20", "GU20", "GU21",
    "SE10", "DN20", "SP20", "GU11", "DN21", "SP21", "GU10", "DN01", "DN10", "RF21", "SE30",
    "RF20", "SP10", "PE00", "GU30", "GU31", "DN30", "SP30", "R221", "R220", "DN31", "SP31",
    "RF31", "RF30", "DN11", "RF10", "SP11", "RF11", "RF00", "R231", "SP01", "RF01", "R230",
    "R210", "R211", "R200", "R201",
)
FAR_STEPS = (1, 3,)


def plan(pairs):
    if pairs == 4:
        return [(word[:-2], int(word[-2]), int(word[-1])) for word in FOUR_PLANES]
    order = [("ZS", step, 0) for step in range(1, pairs)]
    order += [("ZD", step, 0) for step in range(1, pairs)]
    order += [("PS", 0, 0), ("OWN", 0, 0), ("GU", 0, 0), ("GU", 0, 1), ("DN", 0, 0), ("DN", 0, 1)]
    for step in range(1, pairs):
        order += [("SF", step, 0), ("SF", step, 1), ("SS", step, 0), ("SS", step, 1), ("SE", step, 0)]
        order += [("GU", step, 0), ("GU", step, 1), ("DN", step, 0), ("DN", step, 1)]
        order += [("SP", step, 0), ("SP", step, 1), ("RF", step, 0), ("RF", step, 1)]
        order += [("R2", step, 0), ("R2", step, 1)]
    order += [("PE", 0, 0), ("SP", 0, 0), ("SP", 0, 1), ("RF", 0, 0), ("RF", 0, 1)]
    return order + [("R2", 0, 0), ("R2", 0, 1)]


def expert_kernel(
    sizes,
    routes_hbm,
    logits_hbm,
    gain_hbm,
    pool_gain_hbm,
    pool_scale_hbm,
    tokens_hbm,
    gate_hbm,
    up_hbm,
    down_hbm,
    pool_in_hbm,
    pool_weight_hbm,
    out_ref,
    pool_out_ref,
    routes_ref,
    logits_ref,
    gain_ref,
    pool_gain_ref,
    pool_scale_ref,
    tokens_ref,
    pool_in_ref,
    pool_weight_ref,
    rank_ref,
    blend_ref,
    normed,
    outgoing,
    outgoing_far,
    sibling_out,
    rows_in,
    hidden_ref,
    parts,
    first_in0,
    first_in1,
    half_sum0,
    half_sum1,
    second_in0,
    second_in1,
    finished,
    returned,
    gate_ref,
    up_ref,
    down_ref,
    pool_own,
    pool_tail,
    pool_halo,
    load_sem,
    halo_sem,
    go_send,
    go_recv,
    far_send,
    spread_send,
    spread_recv,
    ra0_send,
    ra0_recv,
    ra1_send,
    ra1_recv,
    rb0_send,
    rb0_recv,
    rb1_send,
    rb1_recv,
    back_send,
    back_recv,
):
    experts, ny, nx, slots, columns = sizes
    pairs = experts // 2
    me, shard = lax.axis_index("ep"), lax.axis_index("tp")
    my_pair, my_core = me // 2, me % 2
    my_y, my_x = shard // nx, shard % nx
    bf16, f32 = jnp.bfloat16, jnp.float32
    pending = []

    def device_at(ep, y, x):
        return {"ep": ep, "tp": y * nx + x}

    def copy_to(src, dst, send, recv, target):
        return pltpu.make_async_remote_copy(
            src_ref=src,
            dst_ref=dst,
            send_sem=send,
            recv_sem=recv,
            device_id=target,
            device_id_type=pl.DeviceIdType.MESH,
        )

    def start(*arguments):
        copy = copy_to(*arguments)
        copy.start()
        pending.append(copy)

    def arrive(ref, send, recv):
        copy_to(ref, ref, send, recv, device_at(me, my_y, my_x)).wait_recv()

    others_x = [lax.rem(my_x + step, nx) for step in range(1, nx)]
    others_y = [lax.rem(my_y + step, ny) for step in range(1, ny)]
    barrier = pltpu.get_barrier_semaphore()
    greeted = [device_at(lax.rem(me + step, experts), my_y, my_x) for step in range(1, experts)]
    greeted += [device_at(me, my_y, x) for x in others_x]
    greeted += [device_at(me, y, my_x) for y in others_y]
    for target in greeted:
        pl.semaphore_signal(
            barrier, inc=1, device_id=target, device_id_type=pl.DeviceIdType.MESH
        )
    loads = [
        pltpu.make_async_copy(source, target, load_sem.at[number])
        for number, (source, target) in enumerate(
            (
                (routes_hbm, routes_ref),
                (gain_hbm, gain_ref),
                (logits_hbm, logits_ref),
                (pool_gain_hbm, pool_gain_ref),
                (pool_scale_hbm, pool_scale_ref),
                (tokens_hbm, tokens_ref),
                (gate_hbm.at[0], gate_ref),
                (up_hbm.at[0], up_ref),
                (down_hbm.at[0], down_ref),
                (pool_in_hbm, pool_in_ref),
                (pool_weight_hbm, pool_weight_ref),
            )
        )
    ]
    load_small = loads[:5]
    load_tokens, load_gate, load_up, load_down, load_pool_in, load_pool_weight = loads[5:]
    for copy in load_small:
        copy.start()
    load_tokens.start()
    load_pool_in.start()
    load_gate.start()
    load_up.start()
    load_down.start()
    load_pool_weight.start()

    is_plane = [
        1 - ((my_pair - p) * (my_pair - p) + pairs * pairs - 1) // (pairs * pairs)
        for p in range(pairs)
    ]
    orders = plane_orders(pairs)
    pair_of = [my_pair]
    for step in range(1, pairs):
        number = 0
        for p in range(pairs):
            if orders[p][step - 1]:
                number = number + is_plane[p] * orders[p][step - 1]
        pair_of.append(number)

    for copy in load_small:
        copy.wait()
    tokens_count, picks = routes_ref.shape[1], routes_ref.shape[0]
    expert_ids = lax.broadcasted_iota(jnp.int32, (experts, tokens_count), 0)
    named = [
        jnp.where(routes_ref[pick : pick + 1, :] == expert_ids, 1.0, 0.0) for pick in range(picks)
    ]
    visits = functools.reduce(jnp.add, named)
    earlier = (
        lax.broadcasted_iota(jnp.int32, (tokens_count, tokens_count), 0)
        < lax.broadcasted_iota(jnp.int32, (tokens_count, tokens_count), 1)
    )
    rank = jnp.dot(
        visits.astype(bf16), jnp.where(earlier, 1.0, 0.0).astype(bf16), preferred_element_type=f32
    )
    rank_ref[...] = jnp.where(visits > 0.5, rank, -1.0)
    slot_ids = lax.broadcasted_iota(jnp.int32, (slots, tokens_count), 0).astype(f32)

    def select(expert):
        return jnp.where(rank_ref[pl.ds(expert, 1), :] == slot_ids, 1.0, 0.0)

    def select_two(first, second):
        return jnp.concatenate([select(first), select(second)], axis=0).astype(bf16)

    load_tokens.wait()
    values = tokens_ref[...].astype(f32)
    scale = lax.rsqrt(jnp.mean(values * values, axis=-1, keepdims=True) + EPSILON)
    normed[...] = (values * scale * gain_ref[...]).astype(bf16)
    own_columns = pl.ds(pl.multiple_of(shard * columns, columns), columns)
    far_of = [(y, x) for y in others_y for x in others_x]

    def columns_of(y, x):
        return pl.ds(pl.multiple_of((y * nx + x) * columns, columns), columns)

    for step in range(1, pairs):
        pair = pair_of[step]
        chosen_rows = select_two(pair * 2, pair * 2 + 1)
        targets = [(own_columns, outgoing)]
        if step in FAR_STEPS:
            targets += [
                (columns_of(y, x), outgoing_far.at[number]) for number, (y, x) in enumerate(far_of)
            ]
        for where, target in targets:
            picked = jnp.dot(
                chosen_rows, normed[:, where], preferred_element_type=f32
            ).astype(bf16)
            target[pair * 2] = picked[:slots]
            target[pair * 2 + 1] = picked[slots:]
    sibling = my_pair * 2 + 1 - my_core
    for_both = jnp.dot(
        select_two(sibling, me), normed[...], preferred_element_type=f32
    ).astype(bf16)
    my_rows = pl.ds(pl.multiple_of(my_core * slots, slots), slots)
    for y in range(ny):
        for x in range(nx):
            begin = (y * nx + x) * columns
            sibling_out[y, x] = for_both[:slots, begin : begin + columns]
            rows_in[my_pair, y, x, my_rows, :] = for_both[slots:, begin : begin + columns]
    pl.semaphore_wait(barrier, len(greeted))

    start(
        sibling_out,
        rows_in.at[my_pair, :, :, my_rows],
        go_send.at[sibling],
        go_recv.at[me],
        device_at(sibling, my_y, my_x),
    )

    group_width = pool_weight_ref.shape[0]
    group = shard * pool_weight_ref.shape[1] // group_width
    pool_rows = pool_in_ref.shape[0]
    halo_count = pool_tail.shape[0]

    def pool_start(*_):
        load_pool_in.wait()
        inputs = pool_in_ref[...].astype(f32)
        spread = lax.rsqrt(jnp.mean(inputs * inputs, axis=-1, keepdims=True) + EPSILON)
        group_columns = pl.ds(pl.multiple_of(group * group_width, group_width), group_width)
        own = pool_in_ref[:, group_columns].astype(f32)
        pool_own[...] = (own * spread * pool_gain_ref[:, group_columns]).astype(bf16)
        pool_tail[...] = pool_own[pool_rows - halo_count :, :]
        start(
            pool_tail,
            pool_halo,
            halo_sem.at[0],
            halo_sem.at[1],
            device_at(lax.rem(me + 1, experts), my_y, my_x),
        )
        raised = jnp.exp(logits_ref[...])
        shares = raised / jnp.sum(raised, axis=0, keepdims=True)
        share_of = functools.reduce(
            jnp.add, [named[pick] * shares[pick : pick + 1, :] for pick in range(picks)]
        )
        weighted = [
            jnp.where(rank_ref[e : e + 1, :] == slot_ids, share_of[e : e + 1, :], 0.0)
            for e in range(experts)
        ]
        blend_ref[...] = jnp.concatenate(weighted, axis=0).T.astype(bf16)

    def pool_end(*_):
        load_pool_weight.wait()
        arrive(pool_halo, halo_sem.at[0], halo_sem.at[1])
        own = pool_own[...].astype(f32)
        halo = jnp.where(me == 0, 0.0, pool_halo[...].astype(f32))
        current = jnp.concatenate([halo, own], axis=0)
        chosen = jnp.zeros_like(current)
        for number in range(4):
            current = current + pltpu.roll(current, 1 << number, 0)
            chosen = jnp.where(group == number, current, chosen)
        window = jnp.where(group == 0, 2, jnp.where(group == 1, 4, jnp.where(group == 2, 8, 16)))
        position = me * pool_rows + lax.broadcasted_iota(jnp.int32, (pool_rows, 1), 0)
        counts = jnp.minimum(position + 1, window).astype(f32)
        mixed = (chosen[halo_count:] / counts - own).astype(bf16)
        product = jnp.dot(mixed, pool_weight_ref[...], preferred_element_type=f32)
        pool_out_ref[...] = (product * pool_scale_ref[...]).astype(bf16)

    sibling_rows = pl.ds(pl.multiple_of((1 - my_core) * slots, slots), slots)

    def rows_of(core):
        return pl.ds(core * slots, slots)

    def own_rows(*_):
        arrive(
            rows_in.at[my_pair, :, :, sibling_rows], go_send.at[sibling], go_recv.at[sibling]
        )
        load_gate.wait()
        load_up.wait()

    def spread_recv_of(pair, core, y, x):
        return spread_recv.at[(pair * 2 + core) * ny + y, x]

    def spread_send_of(pair, core, y, x):
        return spread_send.at[(pair * 2 + core) * ny + y, x]

    def go_own(step, _):
        for core in range(2):
            expert = pair_of[step] * 2 + core
            start(
                outgoing.at[expert],
                rows_in.at[my_pair, my_y, my_x, my_rows],
                go_send.at[expert],
                go_recv.at[me],
                device_at(expert, my_y, my_x),
            )

    def go_far(step, _):
        if step not in FAR_STEPS:
            return
        for core in range(2):
            expert = pair_of[step] * 2 + core
            for number, (y, x) in enumerate(far_of):
                start(
                    outgoing_far.at[number, expert],
                    rows_in.at[my_pair, y, x, my_rows],
                    far_send.at[number, expert],
                    spread_recv.at[me * ny + y, x],
                    device_at(expert, my_y, my_x),
                )

    def spread_own(step, core):
        pair = pair_of[step]
        block = rows_in.at[pair, my_y, my_x, rows_of(core)]
        source = pair * 2 + core
        arrive(block, go_send.at[source], go_recv.at[source])
        mine = spread_recv_of(pair, core, my_y, my_x)
        for x in others_x:
            start(block, block, spread_send_of(pair, core, my_y, x), mine, device_at(me, my_y, x))
        for y in others_y:
            start(block, block, spread_send_of(pair, core, y, my_x), mine, device_at(me, y, my_x))

    def take(step, core, y, x):
        pair = pair_of[step]
        arrive(
            rows_in.at[pair, y, x, rows_of(core)],
            spread_send_of(pair, core, y, x),
            spread_recv_of(pair, core, y, x),
        )

    def relay(step, core):
        pair = pair_of[step]
        if step in FAR_STEPS:
            return
        if core == 0:
            for x in others_x:
                take(step, core, my_y, x)
                block = rows_in.at[pair, my_y, x, rows_of(core)]
                arrived = spread_recv_of(pair, core, my_y, x)
                for y in others_y:
                    start(block, block, spread_send_of(pair, core, y, x), arrived, device_at(me, y, my_x))
        else:
            for y in others_y:
                take(step, core, y, my_x)
                block = rows_in.at[pair, y, my_x, rows_of(core)]
                arrived = spread_recv_of(pair, core, y, my_x)
                for x in others_x:
                    start(block, block, spread_send_of(pair, core, y, x), arrived, device_at(me, my_y, x))

    def spread_end(step, _):
        for core in range(2):
            relayed = step not in FAR_STEPS
            if not (relayed and core == 0):
                for x in others_x:
                    take(step, core, my_y, x)
            if not (relayed and core == 1):
                for y in others_y:
                    take(step, core, y, my_x)
            for y, x in far_of:
                take(step, core, y, x)

    hidden_half = gate_ref.shape[1] // 2

    def gate_up(step, half):
        pair = pair_of[step]
        entire = jnp.concatenate(
            [rows_in[pair, y, x] for y in range(ny) for x in range(nx)], axis=1
        )
        where = pl.ds(half * hidden_half, hidden_half)
        gate_part = jnp.dot(entire, gate_ref[:, where], preferred_element_type=f32)
        up_part = jnp.dot(entire, up_ref[:, where], preferred_element_type=f32)
        hidden_ref[step, :, where] = (
            gate_part / (1.0 + jnp.exp(-gate_part)) * up_part
        ).astype(bf16)

    def down(step, part):
        pair = pair_of[step]
        if step == 0 and part == 0:
            load_down.wait()
        hidden = hidden_ref[step]
        blocks = far_of
        if part:
            blocks = [(my_y, x) for x in others_x] + [(y, my_x) for y in others_y] + [(my_y, my_x)]
        for y, x in blocks:
            parts[pair, y, x] = lax.dot_general(
                hidden,
                down_ref[columns_of(y, x), :],
                (((1,), (1,)), ((), ())),
                preferred_element_type=f32,
            ).astype(bf16)

    def send_parts(step, part):
        pair = pair_of[step]
        for y in [my_y] if part else others_y:
            for x in others_x:
                start(
                    parts.at[pair, y, x, rows_of(0)],
                    first_in0.at[pair, my_x, y],
                    ra0_send.at[pair * nx + x, y],
                    ra0_recv.at[pair * nx + my_x, y],
                    device_at(me, my_y, x),
                )
        for x in [my_x] if part else others_x:
            for y in others_y:
                start(
                    parts.at[pair, y, x, rows_of(1)],
                    first_in1.at[pair, my_y, x],
                    ra1_send.at[pair * ny + y, x],
                    ra1_recv.at[pair * ny + my_y, x],
                    device_at(me, y, my_x),
                )

    def summed0(pair, y):
        total = parts[pair, y, my_x, rows_of(0), :].astype(f32)
        for x in others_x:
            arrive(
                first_in0.at[pair, x, y], ra0_send.at[pair * nx + x, y], ra0_recv.at[pair * nx + x, y]
            )
            total += first_in0[pair, x, y].astype(f32)
        return total

    def summed1(pair, x):
        total = parts[pair, my_y, x, rows_of(1), :].astype(f32)
        for y in others_y:
            arrive(
                first_in1.at[pair, y, x], ra1_send.at[pair * ny + y, x], ra1_recv.at[pair * ny + y, x]
            )
            total += first_in1[pair, y, x].astype(f32)
        return total

    def reduce_first(step, core):
        pair = pair_of[step]
        if core == 0:
            for y in others_y:
                half_sum0[pair, y] = summed0(pair, y).astype(bf16)
                start(
                    half_sum0.at[pair, y],
                    second_in0.at[pair, my_y],
                    rb0_send.at[pair, y],
                    rb0_recv.at[pair, my_y],
                    device_at(me, y, my_x),
                )
        else:
            for x in others_x:
                half_sum1[pair, x] = summed1(pair, x).astype(bf16)
                start(
                    half_sum1.at[pair, x],
                    second_in1.at[pair, my_x],
                    rb1_send.at[pair, x],
                    rb1_recv.at[pair, my_x],
                    device_at(me, my_y, x),
                )

    def slots_of(expert):
        return pl.ds(pl.multiple_of(expert * slots, slots), slots)

    def give_back(target):
        start(
            finished.at[target],
            returned.at[slots_of(me)],
            back_send.at[target],
            back_recv.at[me],
            device_at(target, my_y, my_x),
        )

    def reduce_second(step, core):
        pair = pair_of[step]
        if core == 0:
            total = summed0(pair, my_y)
            for y in others_y:
                arrive(second_in0.at[pair, y], rb0_send.at[pair, y], rb0_recv.at[pair, y])
                total += second_in0[pair, y].astype(f32)
        else:
            total = summed1(pair, my_x)
            for x in others_x:
                arrive(second_in1.at[pair, x], rb1_send.at[pair, x], rb1_recv.at[pair, x])
                total += second_in1[pair, x].astype(f32)
        finished[pair * 2 + core] = total.astype(bf16)
        if step:
            give_back(pair * 2 + core)
        elif core:
            give_back(sibling)
            returned[slots_of(me), :] = finished[me]

    actions = {
        "ZS": go_own,
        "ZD": go_far,
        "PS": pool_start,
        "PE": pool_end,
        "OWN": own_rows,
        "SF": spread_own,
        "SS": relay,
        "SE": spread_end,
        "GU": gate_up,
        "DN": down,
        "SP": send_parts,
        "RF": reduce_first,
        "R2": reduce_second,
    }
    for name, step, part in plan(pairs):
        actions[name](step, part)
    for step in range(1, experts):
        source = lax.rem(me + step, experts)
        arrive(returned.at[slots_of(source)], back_send.at[source], back_recv.at[source])
    out_ref[...] = jnp.dot(blend_ref[...], returned[...], preferred_element_type=f32).astype(bf16)
    for copy in pending:
        copy.wait_send()


def local(
    pool_input,
    pool_gain,
    pool_weight,
    pool_scale,
    moe_input,
    moe_gain,
    routes,
    route_logits,
    gate_weight,
    up_weight,
    down_weight,
):
    local_rows, row_width = moe_input.shape
    picks_count = routes.shape[1]
    experts, shards = lax.axis_size("ep"), lax.axis_size("tp")
    capacity = 2 * local_rows * picks_count // experts
    slots = -(-capacity // 16) * 16
    columns = row_width // shards
    ny = max(d for d in range(1, shards + 1) if shards % d == 0 and d * d <= shards)
    nx = shards // ny
    pairs = experts // 2
    hidden_units = gate_weight.shape[2]
    pool_rows, group_width = pool_input.shape[0], pool_weight.shape[0]

    bf16, f32 = jnp.bfloat16, jnp.float32
    dma = pltpu.SemaphoreType.DMA
    vmem = pl.BlockSpec(memory_space=pltpu.VMEM)
    anywhere = pl.BlockSpec(memory_space=pl.ANY)
    block = (slots, columns)
    sems_x, sems_y = dma((pairs, nx)), dma((pairs, ny))
    spread_sems = dma((experts * ny, nx))
    far_count = (ny - 1) * (nx - 1)
    expert_out, pool_out = pl.pallas_call(
        functools.partial(expert_kernel, (experts, ny, nx, slots, columns)),
        out_shape=(
            pltpu.VMEM((local_rows, columns), bf16),
            pltpu.VMEM((pool_rows, pool_weight.shape[1]), bf16),
        ),
        in_specs=[anywhere] * 11,
        out_specs=(vmem, vmem),
        scratch_shapes=[
            pltpu.VMEM((picks_count, local_rows), jnp.int32),
            pltpu.VMEM((picks_count, local_rows), f32),
            pltpu.VMEM((1, row_width), f32),
            pltpu.VMEM((1, row_width), f32),
            pltpu.VMEM((1, pool_weight.shape[1]), f32),
            pltpu.VMEM((local_rows, row_width), bf16),
            pltpu.VMEM((pool_rows, row_width), bf16),
            pltpu.VMEM(pool_weight.shape, bf16),
            pltpu.VMEM((experts, local_rows), f32),
            pltpu.VMEM((local_rows, experts * slots), bf16),
            pltpu.VMEM((local_rows, row_width), bf16),
            pltpu.VMEM((experts,) + block, bf16),
            pltpu.VMEM((far_count, experts) + block, bf16),
            pltpu.VMEM((ny, nx) + block, bf16),
            pltpu.VMEM((pairs, ny, nx, 2 * slots, columns), bf16),
            pltpu.VMEM((pairs, 2 * slots, hidden_units), bf16),
            pltpu.VMEM((pairs, ny, nx, 2 * slots, columns), bf16),
            pltpu.VMEM((pairs, nx, ny) + block, bf16),
            pltpu.VMEM((pairs, ny, nx) + block, bf16),
            pltpu.VMEM((pairs, ny) + block, bf16),
            pltpu.VMEM((pairs, nx) + block, bf16),
            pltpu.VMEM((pairs, ny) + block, bf16),
            pltpu.VMEM((pairs, nx) + block, bf16),
            pltpu.VMEM((experts,) + block, bf16),
            pltpu.VMEM((experts * slots, columns), bf16),
            pltpu.VMEM((row_width, hidden_units), bf16),
            pltpu.VMEM((row_width, hidden_units), bf16),
            pltpu.VMEM((row_width, hidden_units), bf16),
            pltpu.VMEM((pool_rows, group_width), bf16),
            pltpu.VMEM((halo_rows, group_width), bf16),
            pltpu.VMEM((halo_rows, group_width), bf16),
            dma((11,)),
            dma((2,)),
            dma((experts,)),
            dma((experts,)),
        ]
        + [dma((far_count, experts)), spread_sems, spread_sems]
        + [dma((pairs * nx, ny))] * 2
        + [dma((pairs * ny, nx))] * 2
        + [sems_y, sems_y, sems_x, sems_x]
        + [dma((experts,)), dma((experts,))],
        compiler_params=pltpu.CompilerParams(
            collective_id=0, has_side_effects=True, vmem_limit_bytes=56 * 1024 * 1024
        ),
    )(
        routes.T,
        route_logits.T,
        moe_gain.reshape(1, row_width),
        pool_gain.reshape(1, row_width),
        pool_scale.reshape(1, -1),
        moe_input,
        gate_weight,
        up_weight,
        down_weight,
        pool_input,
        pool_weight,
    )
    return (pool_out, expert_out)


def solution(mesh):
    in_specs = (
        P("ep", None),
        P(),
        P(None, "tp"),
        P("tp"),
        P("ep", None),
        P(),
        P("ep", None),
        P("ep", None),
        P("ep", None, "tp"),
        P("ep", None, "tp"),
        P("ep", None, "tp"),
    )
    out_specs = (P("ep", "tp"), P("ep", "tp"))
    return jax.shard_map(local, mesh=mesh, in_specs=in_specs, out_specs=out_specs, check_vma=False)
```

```python
import functools

import jax
import jax.numpy as jnp
from jax import lax
from jax.experimental import pallas as pl
from jax.experimental.pallas import tpu as pltpu
from jax.sharding import PartitionSpec as P

EPSILON = 1e-06
halo_rows = 16


def plane_orders(planes):
    if planes == 4:
        return [[1, 3, 2], [0, 2, 3], [3, 1, 0], [2, 0, 1]]
    return [[(p + step) % planes for step in range(1, planes)] for p in range(planes)]


FOUR_PLANES = (
    "ZS10", "ZS20", "PS00", "ZS30", "SB00", "SF11", "OWN00", "ZD10", "GU01", "SF10", "SF21",
    "GU00", "SF20", "DN00", "SP00", "SS21", "SS20", "SF31", "ZD30", "SF30", "SE20", "GU20",
    "GU21", "SE10", "DN20", "GU11", "SP20", "DN21", "SP21", "GU10", "DN01", "DN10", "RF21",
    "RF20", "SE30", "SP10", "GU30", "DN11", "GU31", "DN30", "SP30", "R221", "R220", "DN31",
    "SP31", "RF31", "RF30", "RF10", "SP11", "RF11", "PE00", "RF00", "R231", "SP01", "RF01",
    "R210", "R230", "R211", "R200", "R201",
)
FAR_STEPS = (1, 3)


def plan(pairs):
    if pairs == 4:
        return [(word[:-2], int(word[-2]), int(word[-1])) for word in FOUR_PLANES]
    order = [("ZS", step, 0) for step in range(1, pairs)]
    order += [("SB", 0, 0)] + [("ZD", step, 0) for step in range(1, pairs)]
    order += [("PS", 0, 0), ("OWN", 0, 0), ("GU", 0, 0), ("GU", 0, 1), ("DN", 0, 0), ("DN", 0, 1)]
    for step in range(1, pairs):
        order += [("SF", step, 0), ("SF", step, 1), ("SS", step, 0), ("SS", step, 1), ("SE", step, 0)]
        order += [("GU", step, 0), ("GU", step, 1), ("DN", step, 0), ("DN", step, 1)]
        order += [("SP", step, 0), ("SP", step, 1), ("RF", step, 0), ("RF", step, 1)]
        order += [("R2", step, 0), ("R2", step, 1)]
    order += [("PE", 0, 0), ("SP", 0, 0), ("SP", 0, 1), ("RF", 0, 0), ("RF", 0, 1)]
    return order + [("R2", 0, 0), ("R2", 0, 1)]


def expert_kernel(
    sizes,
    routes_hbm,
    logits_hbm,
    gain_hbm,
    pool_gain_hbm,
    pool_scale_hbm,
    tokens_hbm,
    gate_hbm,
    up_hbm,
    down_hbm,
    pool_in_hbm,
    pool_weight_hbm,
    out_ref,
    pool_out_ref,
    routes_ref,
    logits_ref,
    gain_ref,
    pool_gain_ref,
    pool_scale_ref,
    tokens_ref,
    pool_in_ref,
    pool_weight_ref,
    rank_ref,
    blend_ref,
    normed,
    outgoing,
    outgoing_far,
    sibling_out,
    rows_in,
    hidden_ref,
    parts,
    first_in0,
    first_in1,
    half_sum0,
    half_sum1,
    second_in0,
    second_in1,
    own_in0,
    own_in1,
    own_part,
    own_came,
    finished,
    returned,
    gate_ref,
    up_ref,
    down_ref,
    pool_own,
    pool_tail,
    pool_halo,
    load_sem,
    halo_sem,
    go_send,
    go_recv,
    far_send,
    spread_send,
    spread_recv,
    ra0_send,
    ra0_recv,
    ra1_send,
    ra1_recv,
    rb0_send,
    rb0_recv,
    rb1_send,
    rb1_recv,
    own0_send,
    own0_recv,
    own1_send,
    own1_recv,
    core_sem,
    back_send,
    back_recv,
):
    experts, ny, nx, slots, columns = sizes
    pairs = experts // 2
    far_steps = FAR_STEPS if pairs == 4 else ()
    me, shard = lax.axis_index("ep"), lax.axis_index("tp")
    my_pair, my_core = me // 2, me % 2
    my_y, my_x = shard // nx, shard % nx
    bf16, f32 = jnp.bfloat16, jnp.float32
    pending = []

    def device_at(ep, y, x):
        return {"ep": ep, "tp": y * nx + x}

    def copy_to(src, dst, send, recv, target):
        return pltpu.make_async_remote_copy(
            src_ref=src,
            dst_ref=dst,
            send_sem=send,
            recv_sem=recv,
            device_id=target,
            device_id_type=pl.DeviceIdType.MESH,
        )

    def start(*arguments):
        copy = copy_to(*arguments)
        copy.start()
        pending.append(copy)

    def arrive(ref, send, recv):
        copy_to(ref, ref, send, recv, device_at(me, my_y, my_x)).wait_recv()

    others_x = [lax.rem(my_x + step, nx) for step in range(1, nx)]
    others_y = [lax.rem(my_y + step, ny) for step in range(1, ny)]
    barrier = pltpu.get_barrier_semaphore()
    greeted = [device_at(lax.rem(me + step, experts), my_y, my_x) for step in range(1, experts)]
    for ep in (me, my_pair * 2 + 1 - my_core):
        greeted += [device_at(ep, my_y, x) for x in others_x]
        greeted += [device_at(ep, y, my_x) for y in others_y]
    for target in greeted:
        pl.semaphore_signal(
            barrier, inc=1, device_id=target, device_id_type=pl.DeviceIdType.MESH
        )
    loads = [
        pltpu.make_async_copy(source, target, load_sem.at[number])
        for number, (source, target) in enumerate(
            (
                (routes_hbm, routes_ref),
                (gain_hbm, gain_ref),
                (logits_hbm, logits_ref),
                (pool_gain_hbm, pool_gain_ref),
                (pool_scale_hbm, pool_scale_ref),
                (tokens_hbm, tokens_ref),
                (gate_hbm.at[0], gate_ref),
                (up_hbm.at[0], up_ref),
                (down_hbm.at[0], down_ref),
                (pool_in_hbm, pool_in_ref),
                (pool_weight_hbm, pool_weight_ref),
            )
        )
    ]
    load_small = loads[:5]
    load_tokens, load_gate, load_up, load_down, load_pool_in, load_pool_weight = loads[5:]
    for copy in load_small:
        copy.start()
    load_tokens.start()
    load_pool_in.start()
    load_gate.start()
    load_up.start()
    load_down.start()
    load_pool_weight.start()

    is_plane = [
        1 - ((my_pair - p) * (my_pair - p) + pairs * pairs - 1) // (pairs * pairs)
        for p in range(pairs)
    ]
    orders = plane_orders(pairs)
    pair_of = [my_pair]
    for step in range(1, pairs):
        number = 0
        for p in range(pairs):
            if orders[p][step - 1]:
                number = number + is_plane[p] * orders[p][step - 1]
        pair_of.append(number)

    for copy in load_small:
        copy.wait()
    tokens_count, picks = routes_ref.shape[1], routes_ref.shape[0]
    expert_ids = lax.broadcasted_iota(jnp.int32, (experts, tokens_count), 0)
    named = [
        jnp.where(routes_ref[pick : pick + 1, :] == expert_ids, 1.0, 0.0) for pick in range(picks)
    ]
    visits = functools.reduce(jnp.add, named)
    earlier = (
        lax.broadcasted_iota(jnp.int32, (tokens_count, tokens_count), 0)
        < lax.broadcasted_iota(jnp.int32, (tokens_count, tokens_count), 1)
    )
    rank = jnp.dot(
        visits.astype(bf16), jnp.where(earlier, 1.0, 0.0).astype(bf16), preferred_element_type=f32
    )
    rank_ref[...] = jnp.where(visits > 0.5, rank, -1.0)
    slot_ids = lax.broadcasted_iota(jnp.int32, (slots, tokens_count), 0).astype(f32)

    def select(expert):
        return jnp.where(rank_ref[pl.ds(expert, 1), :] == slot_ids, 1.0, 0.0)

    def select_two(first, second):
        return jnp.concatenate([select(first), select(second)], axis=0).astype(bf16)

    load_tokens.wait()
    values = tokens_ref[...].astype(f32)
    scale = lax.rsqrt(jnp.mean(values * values, axis=-1, keepdims=True) + EPSILON)
    normed[...] = (values * scale * gain_ref[...]).astype(bf16)
    own_columns = pl.ds(pl.multiple_of(shard * columns, columns), columns)
    far_of = [(y, x) for y in others_y for x in others_x]

    def columns_of(y, x):
        return pl.ds(pl.multiple_of((y * nx + x) * columns, columns), columns)

    sibling = my_pair * 2 + 1 - my_core
    my_rows = pl.ds(pl.multiple_of(my_core * slots, slots), slots)
    pl.semaphore_wait(barrier, len(greeted))

    def pick_rows(step, columns_at, target):
        pair = pair_of[step]
        picked = jnp.dot(
            select_two(pair * 2, pair * 2 + 1),
            normed[:, columns_at],
            preferred_element_type=f32,
        ).astype(bf16)
        target[pair * 2] = picked[:slots]
        target[pair * 2 + 1] = picked[slots:]

    def go_sibling(*_):
        for_both = jnp.dot(
            select_two(sibling, me), normed[...], preferred_element_type=f32
        ).astype(bf16)
        for y in range(ny):
            for x in range(nx):
                begin = (y * nx + x) * columns
                sibling_out[y, x] = for_both[:slots, begin : begin + columns]
                rows_in[my_pair, y, x, my_rows, :] = for_both[slots:, begin : begin + columns]
        start(
            sibling_out,
            rows_in.at[my_pair, :, :, my_rows],
            go_send.at[sibling],
            go_recv.at[me],
            device_at(sibling, my_y, my_x),
        )

    group_width = pool_weight_ref.shape[0]
    group = shard * pool_weight_ref.shape[1] // group_width
    pool_rows = pool_in_ref.shape[0]
    halo_count = pool_tail.shape[0]

    def pool_start(*_):
        load_pool_in.wait()
        inputs = pool_in_ref[...].astype(f32)
        spread = lax.rsqrt(jnp.mean(inputs * inputs, axis=-1, keepdims=True) + EPSILON)
        group_columns = pl.ds(pl.multiple_of(group * group_width, group_width), group_width)
        own = pool_in_ref[:, group_columns].astype(f32)
        pool_own[...] = (own * spread * pool_gain_ref[:, group_columns]).astype(bf16)
        pool_tail[...] = pool_own[pool_rows - halo_count :, :]
        start(
            pool_tail,
            pool_halo,
            halo_sem.at[0],
            halo_sem.at[1],
            device_at(lax.rem(me + 1, experts), my_y, my_x),
        )
        raised = jnp.exp(logits_ref[...])
        shares = raised / jnp.sum(raised, axis=0, keepdims=True)
        share_of = functools.reduce(
            jnp.add, [named[pick] * shares[pick : pick + 1, :] for pick in range(picks)]
        )
        weighted = [
            jnp.where(rank_ref[e : e + 1, :] == slot_ids, share_of[e : e + 1, :], 0.0)
            for e in range(experts)
        ]
        blend_ref[...] = jnp.concatenate(weighted, axis=0).T.astype(bf16)

    def pool_end(*_):
        load_pool_weight.wait()
        arrive(pool_halo, halo_sem.at[0], halo_sem.at[1])
        own = pool_own[...].astype(f32)
        halo = jnp.where(me == 0, 0.0, pool_halo[...].astype(f32))
        current = jnp.concatenate([halo, own], axis=0)
        chosen = jnp.zeros_like(current)
        for number in range(4):
            current = current + pltpu.roll(current, 1 << number, 0)
            chosen = jnp.where(group == number, current, chosen)
        window = jnp.where(group == 0, 2, jnp.where(group == 1, 4, jnp.where(group == 2, 8, 16)))
        position = me * pool_rows + lax.broadcasted_iota(jnp.int32, (pool_rows, 1), 0)
        counts = jnp.minimum(position + 1, window).astype(f32)
        mixed = (chosen[halo_count:] / counts - own).astype(bf16)
        product = jnp.dot(mixed, pool_weight_ref[...], preferred_element_type=f32)
        pool_out_ref[...] = (product * pool_scale_ref[...]).astype(bf16)

    sibling_rows = pl.ds(pl.multiple_of((1 - my_core) * slots, slots), slots)

    def rows_of(core):
        return pl.ds(core * slots, slots)

    def own_rows(*_):
        arrive(
            rows_in.at[my_pair, :, :, sibling_rows], go_send.at[sibling], go_recv.at[sibling]
        )
        load_gate.wait()
        load_up.wait()

    def spread_recv_of(pair, core, y, x):
        return spread_recv.at[(pair * 2 + core) * ny + y, x]

    def spread_send_of(pair, core, y, x):
        return spread_send.at[(pair * 2 + core) * ny + y, x]

    def go_own(step, _):
        pick_rows(step, own_columns, outgoing)
        for core in range(2):
            expert = pair_of[step] * 2 + core
            start(
                outgoing.at[expert],
                rows_in.at[my_pair, my_y, my_x, my_rows],
                go_send.at[expert],
                go_recv.at[me],
                device_at(expert, my_y, my_x),
            )

    def go_far(step, _):
        if step not in far_steps:
            return
        for number, (y, x) in enumerate(far_of):
            pick_rows(step, columns_of(y, x), outgoing_far.at[number])
        for core in range(2):
            expert = pair_of[step] * 2 + core
            for number, (y, x) in enumerate(far_of):
                start(
                    outgoing_far.at[number, expert],
                    rows_in.at[my_pair, y, x, my_rows],
                    far_send.at[number, expert],
                    spread_recv.at[me * ny + y, x],
                    device_at(expert, my_y, my_x),
                )

    def spread_own(step, core):
        pair = pair_of[step]
        block = rows_in.at[pair, my_y, my_x, rows_of(core)]
        source = pair * 2 + core
        arrive(block, go_send.at[source], go_recv.at[source])
        mine = spread_recv_of(pair, core, my_y, my_x)
        for x in others_x:
            start(block, block, spread_send_of(pair, core, my_y, x), mine, device_at(me, my_y, x))
        for y in others_y:
            start(block, block, spread_send_of(pair, core, y, my_x), mine, device_at(me, y, my_x))

    def take(step, core, y, x):
        pair = pair_of[step]
        arrive(
            rows_in.at[pair, y, x, rows_of(core)],
            spread_send_of(pair, core, y, x),
            spread_recv_of(pair, core, y, x),
        )

    def relay(step, core):
        pair = pair_of[step]
        if step in far_steps:
            return
        if core == 0:
            for x in others_x:
                take(step, core, my_y, x)
                block = rows_in.at[pair, my_y, x, rows_of(core)]
                arrived = spread_recv_of(pair, core, my_y, x)
                for y in others_y:
                    start(block, block, spread_send_of(pair, core, y, x), arrived, device_at(me, y, my_x))
        else:
            for y in others_y:
                take(step, core, y, my_x)
                block = rows_in.at[pair, y, my_x, rows_of(core)]
                arrived = spread_recv_of(pair, core, y, my_x)
                for x in others_x:
                    start(block, block, spread_send_of(pair, core, y, x), arrived, device_at(me, my_y, x))

    def spread_end(step, _):
        for core in range(2):
            relayed = step not in far_steps
            if not (relayed and core == 0):
                for x in others_x:
                    take(step, core, my_y, x)
            if not (relayed and core == 1):
                for y in others_y:
                    take(step, core, y, my_x)
            for y, x in far_of:
                take(step, core, y, x)

    hidden_half = gate_ref.shape[1] // 2

    def gate_up(step, half):
        pair = pair_of[step]
        entire = jnp.concatenate(
            [rows_in[pair, y, x] for y in range(ny) for x in range(nx)], axis=1
        )
        where = pl.ds(half * hidden_half, hidden_half)
        gate_part = jnp.dot(entire, gate_ref[:, where], preferred_element_type=f32)
        up_part = jnp.dot(entire, up_ref[:, where], preferred_element_type=f32)
        hidden_ref[step, :, where] = (
            gate_part / (1.0 + jnp.exp(-gate_part)) * up_part
        ).astype(bf16)

    def down(step, part):
        pair = pair_of[step]
        if step == 0 and part == 0:
            load_down.wait()
        hidden = hidden_ref[step]
        blocks = far_of
        if part:
            blocks = [(my_y, x) for x in others_x] + [(y, my_x) for y in others_y] + [(my_y, my_x)]
        for y, x in blocks:
            parts[pair, y, x] = lax.dot_general(
                hidden,
                down_ref[columns_of(y, x), :],
                (((1,), (1,)), ((), ())),
                preferred_element_type=f32,
            ).astype(bf16)

    def send_parts(step, part):
        pair = pair_of[step]
        for y in [my_y] if part else others_y:
            for x in others_x:
                start(
                    parts.at[pair, y, x, rows_of(0)],
                    first_in0.at[pair, my_x, y],
                    ra0_send.at[pair * nx + x, y],
                    ra0_recv.at[pair * nx + my_x, y],
                    device_at(me, my_y, x),
                )
        for x in [my_x] if part else others_x:
            for y in others_y:
                start(
                    parts.at[pair, y, x, rows_of(1)],
                    first_in1.at[pair, my_y, x],
                    ra1_send.at[pair * ny + y, x],
                    ra1_recv.at[pair * ny + my_y, x],
                    device_at(me, y, my_x),
                )

    def summed0(pair, y):
        total = parts[pair, y, my_x, rows_of(0), :].astype(f32)
        for x in others_x:
            arrive(
                first_in0.at[pair, x, y], ra0_send.at[pair * nx + x, y], ra0_recv.at[pair * nx + x, y]
            )
            total += first_in0[pair, x, y].astype(f32)
        return total

    def summed1(pair, x):
        total = parts[pair, my_y, x, rows_of(1), :].astype(f32)
        for y in others_y:
            arrive(
                first_in1.at[pair, y, x], ra1_send.at[pair * ny + y, x], ra1_recv.at[pair * ny + y, x]
            )
            total += first_in1[pair, y, x].astype(f32)
        return total

    def reduce_own(core):
        owner = my_pair * 2 + core
        if core == 0:
            others = [(half_sum0, summed0, y, device_at(owner, y, my_x)) for y in others_y]
            arriving, sent, received, here = own_in0, own0_send, own0_recv, my_y
        else:
            others = [(half_sum1, summed1, x, device_at(owner, my_y, x)) for x in others_x]
            arriving, sent, received, here = own_in1, own1_send, own1_recv, my_x
        for sums, summed, place, target in others:
            sums[my_pair, place] = summed(my_pair, place).astype(bf16)
            start(
                sums.at[my_pair, place],
                arriving.at[my_core, here],
                sent.at[place],
                received.at[my_core, here],
                target,
            )

    def keep_own(core):
        mine = summed1(my_pair, my_x) if core else summed0(my_pair, my_y)
        own_part[core] = mine.astype(bf16)

        @pl.when(my_core != core)
        def _():
            copy_to(
                own_part.at[core],
                own_came,
                core_sem.at[0],
                core_sem.at[1],
                device_at(sibling, my_y, my_x),
            ).start()

    def finish_own():
        copy_to(
            own_came, own_came, core_sem.at[0], core_sem.at[1], device_at(me, my_y, my_x)
        ).wait_recv()
        for core in range(2):

            @pl.when(my_core == core)
            def _(core=core):
                arriving, received, sent, places = (
                    (own_in0, own0_recv, own0_send, others_y)
                    if core == 0
                    else (own_in1, own1_recv, own1_send, others_x)
                )
                for source in range(2):
                    part = own_part[core] if source == core else own_came[...]
                    total = part.astype(f32)
                    for place in places:
                        arrive(
                            arriving.at[source, place], sent.at[place], received.at[source, place]
                        )
                        total += arriving[source, place].astype(f32)
                    returned[slots_of(my_pair * 2 + source), :] = total.astype(bf16)

        copy_to(
            own_part.at[0], own_came, core_sem.at[0], core_sem.at[1], device_at(sibling, my_y, my_x)
        ).wait_send()

    def reduce_first(step, core):
        pair = pair_of[step]
        if step == 0:
            reduce_own(core)
        elif core == 0:
            for y in others_y:
                half_sum0[pair, y] = summed0(pair, y).astype(bf16)
                start(
                    half_sum0.at[pair, y],
                    second_in0.at[pair, my_y],
                    rb0_send.at[pair, y],
                    rb0_recv.at[pair, my_y],
                    device_at(me, y, my_x),
                )
        else:
            for x in others_x:
                half_sum1[pair, x] = summed1(pair, x).astype(bf16)
                start(
                    half_sum1.at[pair, x],
                    second_in1.at[pair, my_x],
                    rb1_send.at[pair, x],
                    rb1_recv.at[pair, my_x],
                    device_at(me, my_y, x),
                )

    def slots_of(expert):
        return pl.ds(pl.multiple_of(expert * slots, slots), slots)

    def give_back(target):
        start(
            finished.at[target],
            returned.at[slots_of(me)],
            back_send.at[target],
            back_recv.at[me],
            device_at(target, my_y, my_x),
        )

    def reduce_second(step, core):
        pair = pair_of[step]
        if step == 0:
            if core == 0:
                keep_own(0)
                keep_own(1)
            else:
                finish_own()
            return
        if core == 0:
            total = summed0(pair, my_y)
            for y in others_y:
                arrive(second_in0.at[pair, y], rb0_send.at[pair, y], rb0_recv.at[pair, y])
                total += second_in0[pair, y].astype(f32)
        else:
            total = summed1(pair, my_x)
            for x in others_x:
                arrive(second_in1.at[pair, x], rb1_send.at[pair, x], rb1_recv.at[pair, x])
                total += second_in1[pair, x].astype(f32)
        finished[pair * 2 + core] = total.astype(bf16)
        give_back(pair * 2 + core)

    actions = {
        "ZS": go_own,
        "ZD": go_far,
        "SB": go_sibling,
        "PS": pool_start,
        "PE": pool_end,
        "OWN": own_rows,
        "SF": spread_own,
        "SS": relay,
        "SE": spread_end,
        "GU": gate_up,
        "DN": down,
        "SP": send_parts,
        "RF": reduce_first,
        "R2": reduce_second,
    }
    for name, step, part in plan(pairs):
        actions[name](step, part)
    for step in range(1, pairs):
        for core in range(2):
            source = pair_of[step] * 2 + core
            arrive(returned.at[slots_of(source)], back_send.at[source], back_recv.at[source])
    out_ref[...] = jnp.dot(blend_ref[...], returned[...], preferred_element_type=f32).astype(bf16)
    for copy in pending:
        copy.wait_send()


def store_kernel(pool_ref, expert_ref, pool_hbm, expert_hbm, sems):
    copies = [
        pltpu.make_async_copy(source, target, sems.at[number])
        for number, (source, target) in enumerate(
            ((pool_ref, pool_hbm), (expert_ref, expert_hbm))
        )
    ]
    for copy in copies:
        copy.start()
    for copy in copies:
        copy.wait()


def local(
    pool_input,
    pool_gain,
    pool_weight,
    pool_scale,
    moe_input,
    moe_gain,
    routes,
    route_logits,
    gate_weight,
    up_weight,
    down_weight,
):
    local_rows, row_width = moe_input.shape
    picks_count = routes.shape[1]
    experts, shards = lax.axis_size("ep"), lax.axis_size("tp")
    capacity = 2 * local_rows * picks_count // experts
    slots = -(-capacity // 16) * 16
    columns = row_width // shards
    ny = max(d for d in range(1, shards + 1) if shards % d == 0 and d * d <= shards)
    nx = shards // ny
    pairs = experts // 2
    hidden_units = gate_weight.shape[2]
    pool_rows, group_width = pool_input.shape[0], pool_weight.shape[0]

    bf16, f32 = jnp.bfloat16, jnp.float32
    dma = pltpu.SemaphoreType.DMA
    vmem = pl.BlockSpec(memory_space=pltpu.VMEM)
    anywhere = pl.BlockSpec(memory_space=pl.ANY)
    block = (slots, columns)
    sems_x, sems_y = dma((pairs, nx)), dma((pairs, ny))
    spread_sems = dma((experts * ny, nx))
    far_count = (ny - 1) * (nx - 1)
    expert_out, pool_out = pl.pallas_call(
        functools.partial(expert_kernel, (experts, ny, nx, slots, columns)),
        out_shape=(
            pltpu.VMEM((local_rows, columns), bf16),
            pltpu.VMEM((pool_rows, pool_weight.shape[1]), bf16),
        ),
        in_specs=[anywhere] * 11,
        out_specs=(vmem, vmem),
        scratch_shapes=[
            pltpu.VMEM((picks_count, local_rows), jnp.int32),
            pltpu.VMEM((picks_count, local_rows), f32),
            pltpu.VMEM((1, row_width), f32),
            pltpu.VMEM((1, row_width), f32),
            pltpu.VMEM((1, pool_weight.shape[1]), f32),
            pltpu.VMEM((local_rows, row_width), bf16),
            pltpu.VMEM((pool_rows, row_width), bf16),
            pltpu.VMEM(pool_weight.shape, bf16),
            pltpu.VMEM((experts, local_rows), f32),
            pltpu.VMEM((local_rows, experts * slots), bf16),
            pltpu.VMEM((local_rows, row_width), bf16),
            pltpu.VMEM((experts,) + block, bf16),
            pltpu.VMEM((far_count, experts) + block, bf16),
            pltpu.VMEM((ny, nx) + block, bf16),
            pltpu.VMEM((pairs, ny, nx, 2 * slots, columns), bf16),
            pltpu.VMEM((pairs, 2 * slots, hidden_units), bf16),
            pltpu.VMEM((pairs, ny, nx, 2 * slots, columns), bf16),
            pltpu.VMEM((pairs, nx, ny) + block, bf16),
            pltpu.VMEM((pairs, ny, nx) + block, bf16),
            pltpu.VMEM((pairs, ny) + block, bf16),
            pltpu.VMEM((pairs, nx) + block, bf16),
            pltpu.VMEM((pairs, ny) + block, bf16),
            pltpu.VMEM((pairs, nx) + block, bf16),
            pltpu.VMEM((2, ny) + block, bf16),
            pltpu.VMEM((2, nx) + block, bf16),
            pltpu.VMEM((2,) + block, bf16),
            pltpu.VMEM(block, bf16),
            pltpu.VMEM((experts,) + block, bf16),
            pltpu.VMEM((experts * slots, columns), bf16),
            pltpu.VMEM((row_width, hidden_units), bf16),
            pltpu.VMEM((row_width, hidden_units), bf16),
            pltpu.VMEM((row_width, hidden_units), bf16),
            pltpu.VMEM((pool_rows, group_width), bf16),
            pltpu.VMEM((halo_rows, group_width), bf16),
            pltpu.VMEM((halo_rows, group_width), bf16),
            dma((11,)),
            dma((2,)),
            dma((experts,)),
            dma((experts,)),
        ]
        + [dma((far_count, experts)), spread_sems, spread_sems]
        + [dma((pairs * nx, ny))] * 2
        + [dma((pairs * ny, nx))] * 2
        + [sems_y, sems_y, sems_x, sems_x]
        + [dma((ny,)), dma((2, ny)), dma((nx,)), dma((2, nx)), dma((2,))]
        + [dma((experts,)), dma((experts,))],
        compiler_params=pltpu.CompilerParams(
            collective_id=0, has_side_effects=True, vmem_limit_bytes=56 * 1024 * 1024
        ),
    )(
        routes.T,
        route_logits.T,
        moe_gain.reshape(1, row_width),
        pool_gain.reshape(1, row_width),
        pool_scale.reshape(1, -1),
        moe_input,
        gate_weight,
        up_weight,
        down_weight,
        pool_input,
        pool_weight,
    )
    return pl.pallas_call(
        store_kernel,
        out_shape=(
            jax.ShapeDtypeStruct(pool_out.shape, bf16),
            jax.ShapeDtypeStruct(expert_out.shape, bf16),
        ),
        in_specs=[vmem, vmem],
        out_specs=(anywhere, anywhere),
        scratch_shapes=[dma((2,))],
        compiler_params=pltpu.CompilerParams(vmem_limit_bytes=1024 * 1024),
    )(pool_out, expert_out)


def solution(mesh):
    in_specs = (
        P("ep", None),
        P(),
        P(None, "tp"),
        P("tp"),
        P("ep", None),
        P(),
        P("ep", None),
        P("ep", None),
        P("ep", None, "tp"),
        P("ep", None, "tp"),
        P("ep", None, "tp"),
    )
    out_specs = (P("ep", "tp"), P("ep", "tp"))
    return jax.shard_map(local, mesh=mesh, in_specs=in_specs, out_specs=out_specs, check_vma=False)
```

```python
import functools

import jax
import jax.numpy as jnp
from jax import lax
from jax.experimental import pallas as pl
from jax.experimental.pallas import tpu as pltpu
from jax.sharding import PartitionSpec as P

EPSILON = 1e-06
halo_rows = 16


def plane_orders(planes):
    if planes == 4:
        return [[1, 3, 2], [0, 2, 3], [3, 1, 0], [2, 0, 1]]
    return [[(p + step) % planes for step in range(1, planes)] for p in range(planes)]


FOUR_PLANES = (
    "ZS10", "ZS20", "PS00", "ZS30", "SB00", "SF11", "OWN00", "ZD10", "GU01", "SF10", "SF21",
    "GU00", "SF20", "DN00", "SP00", "SS21", "SS20", "SF31", "ZD30", "SF30", "SE20", "GU20",
    "GU21", "SE10", "DN20", "GU11", "SP20", "DN21", "SP21", "GU10", "DN01", "DN10", "RF21",
    "RF20", "SE30", "SP10", "GU30", "DN11", "GU31", "DN30", "SP30", "R221", "R220", "DN31",
    "SP31", "RF31", "RF30", "RF10", "SP11", "RF11", "PE00", "RF00", "R231", "SP01", "RF01",
    "R210", "R230", "R211", "R200", "R201",
)
FAR_STEPS = (1, 3)


def plan(pairs):
    if pairs == 4:
        return [(word[:-2], int(word[-2]), int(word[-1])) for word in FOUR_PLANES]
    order = [("ZS", step, 0) for step in range(1, pairs)]
    order += [("SB", 0, 0)] + [("ZD", step, 0) for step in range(1, pairs)]
    order += [("PS", 0, 0), ("OWN", 0, 0), ("GU", 0, 0), ("GU", 0, 1), ("DN", 0, 0), ("DN", 0, 1)]
    for step in range(1, pairs):
        order += [("SF", step, 0), ("SF", step, 1), ("SS", step, 0), ("SS", step, 1), ("SE", step, 0)]
        order += [("GU", step, 0), ("GU", step, 1), ("DN", step, 0), ("DN", step, 1)]
        order += [("SP", step, 0), ("SP", step, 1), ("RF", step, 0), ("RF", step, 1)]
        order += [("R2", step, 0), ("R2", step, 1)]
    order += [("PE", 0, 0), ("SP", 0, 0), ("SP", 0, 1), ("RF", 0, 0), ("RF", 0, 1)]
    return order + [("R2", 0, 0), ("R2", 0, 1)]


def expert_kernel(
    sizes,
    routes_hbm,
    logits_hbm,
    gain_hbm,
    pool_gain_hbm,
    pool_scale_hbm,
    tokens_hbm,
    gate_hbm,
    up_hbm,
    down_hbm,
    pool_in_hbm,
    pool_weight_hbm,
    out_ref,
    pool_out_ref,
    routes_ref,
    logits_ref,
    gain_ref,
    pool_gain_ref,
    pool_scale_ref,
    tokens_ref,
    pool_in_ref,
    pool_weight_ref,
    rank_ref,
    blend_ref,
    normed,
    outgoing,
    outgoing_far,
    sibling_out,
    rows_in,
    hidden_ref,
    parts,
    first_in0,
    first_in1,
    half_sum0,
    half_sum1,
    second_in0,
    second_in1,
    own_in0,
    own_in1,
    own_part,
    own_came,
    finished,
    returned,
    gate_ref,
    up_ref,
    down_ref,
    pool_own,
    pool_tail,
    pool_halo,
    load_sem,
    halo_sem,
    go_send,
    go_recv,
    far_send,
    spread_send,
    spread_recv,
    ra0_send,
    ra0_recv,
    ra1_send,
    ra1_recv,
    rb0_send,
    rb0_recv,
    rb1_send,
    rb1_recv,
    own0_send,
    own0_recv,
    own1_send,
    own1_recv,
    core_sem,
    back_send,
    back_recv,
):
    experts, ny, nx, slots, columns = sizes
    pairs = experts // 2
    far_steps = FAR_STEPS if pairs == 4 else ()
    me, shard = lax.axis_index("ep"), lax.axis_index("tp")
    my_pair, my_core = me // 2, me % 2
    my_y, my_x = shard // nx, shard % nx
    bf16, f32 = jnp.bfloat16, jnp.float32
    pending = []

    def device_at(ep, y, x):
        return {"ep": ep, "tp": y * nx + x}

    def copy_to(src, dst, send, recv, target):
        return pltpu.make_async_remote_copy(
            src_ref=src,
            dst_ref=dst,
            send_sem=send,
            recv_sem=recv,
            device_id=target,
            device_id_type=pl.DeviceIdType.MESH,
        )

    def start(*arguments):
        copy = copy_to(*arguments)
        copy.start()
        pending.append(copy)

    def arrive(ref, send, recv):
        copy_to(ref, ref, send, recv, device_at(me, my_y, my_x)).wait_recv()

    others_x = [lax.rem(my_x + step, nx) for step in range(1, nx)]
    others_y = [lax.rem(my_y + step, ny) for step in range(1, ny)]
    barrier = pltpu.get_barrier_semaphore()
    greeted = [device_at(lax.rem(me + step, experts), my_y, my_x) for step in range(1, experts)]
    for ep in (me, my_pair * 2 + 1 - my_core):
        greeted += [device_at(ep, my_y, x) for x in others_x]
        greeted += [device_at(ep, y, my_x) for y in others_y]
    for target in greeted:
        pl.semaphore_signal(
            barrier, inc=1, device_id=target, device_id_type=pl.DeviceIdType.MESH
        )
    loads = [
        pltpu.make_async_copy(source, target, load_sem.at[number])
        for number, (source, target) in enumerate(
            (
                (routes_hbm, routes_ref),
                (gain_hbm, gain_ref),
                (logits_hbm, logits_ref),
                (pool_gain_hbm, pool_gain_ref),
                (pool_scale_hbm, pool_scale_ref),
                (tokens_hbm, tokens_ref),
                (gate_hbm.at[0], gate_ref),
                (up_hbm.at[0], up_ref),
                (down_hbm.at[0], down_ref),
                (pool_in_hbm, pool_in_ref),
                (pool_weight_hbm, pool_weight_ref),
            )
        )
    ]
    load_small = loads[:5]
    load_tokens, load_gate, load_up, load_down, load_pool_in, load_pool_weight = loads[5:]
    for copy in load_small:
        copy.start()
    load_tokens.start()
    load_pool_in.start()
    load_gate.start()
    load_up.start()
    load_down.start()
    load_pool_weight.start()

    is_plane = [
        1 - ((my_pair - p) * (my_pair - p) + pairs * pairs - 1) // (pairs * pairs)
        for p in range(pairs)
    ]
    orders = plane_orders(pairs)
    pair_of = [my_pair]
    for step in range(1, pairs):
        number = 0
        for p in range(pairs):
            if orders[p][step - 1]:
                number = number + is_plane[p] * orders[p][step - 1]
        pair_of.append(number)

    for copy in load_small:
        copy.wait()
    tokens_count, picks = routes_ref.shape[1], routes_ref.shape[0]
    expert_ids = lax.broadcasted_iota(jnp.int32, (experts, tokens_count), 0)
    named = [
        jnp.where(routes_ref[pick : pick + 1, :] == expert_ids, 1.0, 0.0) for pick in range(picks)
    ]
    visits = functools.reduce(jnp.add, named)
    earlier = (
        lax.broadcasted_iota(jnp.int32, (tokens_count, tokens_count), 0)
        < lax.broadcasted_iota(jnp.int32, (tokens_count, tokens_count), 1)
    )
    rank = jnp.dot(
        visits.astype(bf16), jnp.where(earlier, 1.0, 0.0).astype(bf16), preferred_element_type=f32
    )
    rank_ref[...] = jnp.where(visits > 0.5, rank, -1.0)
    slot_ids = lax.broadcasted_iota(jnp.int32, (slots, tokens_count), 0).astype(f32)

    def select(expert):
        return jnp.where(rank_ref[pl.ds(expert, 1), :] == slot_ids, 1.0, 0.0)

    def select_two(first, second):
        return jnp.concatenate([select(first), select(second)], axis=0).astype(bf16)

    load_tokens.wait()
    values = tokens_ref[...].astype(f32)
    scale = lax.rsqrt(jnp.mean(values * values, axis=-1, keepdims=True) + EPSILON)
    normed[...] = (values * scale * gain_ref[...]).astype(bf16)
    own_columns = pl.ds(pl.multiple_of(shard * columns, columns), columns)
    far_of = [(y, x) for y in others_y for x in others_x]

    def columns_of(y, x):
        return pl.ds(pl.multiple_of((y * nx + x) * columns, columns), columns)

    sibling = my_pair * 2 + 1 - my_core
    my_rows = pl.ds(pl.multiple_of(my_core * slots, slots), slots)
    pl.semaphore_wait(barrier, len(greeted))

    def pick_rows(step, columns_at, target):
        pair = pair_of[step]
        picked = jnp.dot(
            select_two(pair * 2, pair * 2 + 1),
            normed[:, columns_at],
            preferred_element_type=f32,
        ).astype(bf16)
        target[pair * 2] = picked[:slots]
        target[pair * 2 + 1] = picked[slots:]

    def go_sibling(*_):
        for_both = jnp.dot(
            select_two(sibling, me), normed[...], preferred_element_type=f32
        ).astype(bf16)
        for y in range(ny):
            for x in range(nx):
                begin = (y * nx + x) * columns
                sibling_out[y, x] = for_both[:slots, begin : begin + columns]
                rows_in[my_pair, y, x, my_rows, :] = for_both[slots:, begin : begin + columns]
        start(
            sibling_out,
            rows_in.at[my_pair, :, :, my_rows],
            go_send.at[sibling],
            go_recv.at[me],
            device_at(sibling, my_y, my_x),
        )

    group_width = pool_weight_ref.shape[0]
    group = shard * pool_weight_ref.shape[1] // group_width
    pool_rows = pool_in_ref.shape[0]
    halo_count = pool_tail.shape[0]

    def pool_start(*_):
        load_pool_in.wait()
        inputs = pool_in_ref[...].astype(f32)
        spread = lax.rsqrt(jnp.mean(inputs * inputs, axis=-1, keepdims=True) + EPSILON)
        group_columns = pl.ds(pl.multiple_of(group * group_width, group_width), group_width)
        own = pool_in_ref[:, group_columns].astype(f32)
        pool_own[...] = (own * spread * pool_gain_ref[:, group_columns]).astype(bf16)
        pool_tail[...] = pool_own[pool_rows - halo_count :, :]
        start(
            pool_tail,
            pool_halo,
            halo_sem.at[0],
            halo_sem.at[1],
            device_at(lax.rem(me + 1, experts), my_y, my_x),
        )
        raised = jnp.exp(logits_ref[...])
        shares = raised / jnp.sum(raised, axis=0, keepdims=True)
        share_of = functools.reduce(
            jnp.add, [named[pick] * shares[pick : pick + 1, :] for pick in range(picks)]
        )
        weighted = [
            jnp.where(rank_ref[e : e + 1, :] == slot_ids, share_of[e : e + 1, :], 0.0)
            for e in range(experts)
        ]
        blend_ref[...] = jnp.concatenate(weighted, axis=0).T.astype(bf16)

    def pool_end(*_):
        load_pool_weight.wait()
        arrive(pool_halo, halo_sem.at[0], halo_sem.at[1])
        own = pool_own[...].astype(f32)
        halo = jnp.where(me == 0, 0.0, pool_halo[...].astype(f32))
        current = jnp.concatenate([halo, own], axis=0)
        chosen = jnp.zeros_like(current)
        for number in range(4):
            current = current + pltpu.roll(current, 1 << number, 0)
            chosen = jnp.where(group == number, current, chosen)
        window = jnp.where(group == 0, 2, jnp.where(group == 1, 4, jnp.where(group == 2, 8, 16)))
        position = me * pool_rows + lax.broadcasted_iota(jnp.int32, (pool_rows, 1), 0)
        counts = jnp.minimum(position + 1, window).astype(f32)
        mixed = (chosen[halo_count:] / counts - own).astype(bf16)
        product = jnp.dot(mixed, pool_weight_ref[...], preferred_element_type=f32)
        pool_out_ref[...] = (product * pool_scale_ref[...]).astype(bf16)

    sibling_rows = pl.ds(pl.multiple_of((1 - my_core) * slots, slots), slots)

    def rows_of(core):
        return pl.ds(core * slots, slots)

    def own_rows(*_):
        arrive(
            rows_in.at[my_pair, :, :, sibling_rows], go_send.at[sibling], go_recv.at[sibling]
        )
        load_gate.wait()
        load_up.wait()

    def spread_recv_of(pair, core, y, x):
        return spread_recv.at[(pair * 2 + core) * ny + y, x]

    def spread_send_of(pair, core, y, x):
        return spread_send.at[(pair * 2 + core) * ny + y, x]

    def go_own(step, _):
        pick_rows(step, own_columns, outgoing)
        for core in range(2):
            expert = pair_of[step] * 2 + core
            start(
                outgoing.at[expert],
                rows_in.at[my_pair, my_y, my_x, my_rows],
                go_send.at[expert],
                go_recv.at[me],
                device_at(expert, my_y, my_x),
            )

    def go_far(step, _):
        if step not in far_steps:
            return
        for number, (y, x) in enumerate(far_of):
            pick_rows(step, columns_of(y, x), outgoing_far.at[number])
        for core in range(2):
            expert = pair_of[step] * 2 + core
            for number, (y, x) in enumerate(far_of):
                start(
                    outgoing_far.at[number, expert],
                    rows_in.at[my_pair, y, x, my_rows],
                    far_send.at[number, expert],
                    spread_recv.at[me * ny + y, x],
                    device_at(expert, my_y, my_x),
                )

    def spread_own(step, core):
        pair = pair_of[step]
        block = rows_in.at[pair, my_y, my_x, rows_of(core)]
        source = pair * 2 + core
        arrive(block, go_send.at[source], go_recv.at[source])
        mine = spread_recv_of(pair, core, my_y, my_x)
        for x in others_x:
            start(block, block, spread_send_of(pair, core, my_y, x), mine, device_at(me, my_y, x))
        for y in others_y:
            start(block, block, spread_send_of(pair, core, y, my_x), mine, device_at(me, y, my_x))

    def take(step, core, y, x):
        pair = pair_of[step]
        arrive(
            rows_in.at[pair, y, x, rows_of(core)],
            spread_send_of(pair, core, y, x),
            spread_recv_of(pair, core, y, x),
        )

    def relay(step, core):
        pair = pair_of[step]
        if step in far_steps:
            return
        if core == 0:
            for x in others_x:
                take(step, core, my_y, x)
                block = rows_in.at[pair, my_y, x, rows_of(core)]
                arrived = spread_recv_of(pair, core, my_y, x)
                for y in others_y:
                    start(block, block, spread_send_of(pair, core, y, x), arrived, device_at(me, y, my_x))
        else:
            for y in others_y:
                take(step, core, y, my_x)
                block = rows_in.at[pair, y, my_x, rows_of(core)]
                arrived = spread_recv_of(pair, core, y, my_x)
                for x in others_x:
                    start(block, block, spread_send_of(pair, core, y, x), arrived, device_at(me, my_y, x))

    def spread_end(step, _):
        for core in range(2):
            relayed = step not in far_steps
            if not (relayed and core == 0):
                for x in others_x:
                    take(step, core, my_y, x)
            if not (relayed and core == 1):
                for y in others_y:
                    take(step, core, y, my_x)
            for y, x in far_of:
                take(step, core, y, x)

    hidden_half = gate_ref.shape[1] // 2

    def gate_up(step, half):
        pair = pair_of[step]
        entire = jnp.concatenate(
            [rows_in[pair, y, x] for y in range(ny) for x in range(nx)], axis=1
        )
        where = pl.ds(half * hidden_half, hidden_half)
        gate_part = jnp.dot(entire, gate_ref[:, where], preferred_element_type=f32)
        up_part = jnp.dot(entire, up_ref[:, where], preferred_element_type=f32)
        hidden_ref[step, :, where] = (
            gate_part / (1.0 + jnp.exp(-gate_part)) * up_part
        ).astype(bf16)

    def down(step, part):
        pair = pair_of[step]
        if step == 0 and part == 0:
            load_down.wait()
        hidden = hidden_ref[step]
        blocks = far_of
        if part:
            blocks = [(my_y, x) for x in others_x] + [(y, my_x) for y in others_y] + [(my_y, my_x)]
        for y, x in blocks:
            parts[pair, y, x] = lax.dot_general(
                hidden,
                down_ref[columns_of(y, x), :],
                (((1,), (1,)), ((), ())),
                preferred_element_type=f32,
            ).astype(bf16)

    def send_parts(step, part):
        pair = pair_of[step]
        for y in [my_y] if part else others_y:
            for x in others_x:
                start(
                    parts.at[pair, y, x, rows_of(0)],
                    first_in0.at[pair, my_x, y],
                    ra0_send.at[pair * nx + x, y],
                    ra0_recv.at[pair * nx + my_x, y],
                    device_at(me, my_y, x),
                )
        for x in [my_x] if part else others_x:
            for y in others_y:
                start(
                    parts.at[pair, y, x, rows_of(1)],
                    first_in1.at[pair, my_y, x],
                    ra1_send.at[pair * ny + y, x],
                    ra1_recv.at[pair * ny + my_y, x],
                    device_at(me, y, my_x),
                )

    def summed0(pair, y):
        total = parts[pair, y, my_x, rows_of(0), :].astype(f32)
        for x in others_x:
            arrive(
                first_in0.at[pair, x, y], ra0_send.at[pair * nx + x, y], ra0_recv.at[pair * nx + x, y]
            )
            total += first_in0[pair, x, y].astype(f32)
        return total

    def summed1(pair, x):
        total = parts[pair, my_y, x, rows_of(1), :].astype(f32)
        for y in others_y:
            arrive(
                first_in1.at[pair, y, x], ra1_send.at[pair * ny + y, x], ra1_recv.at[pair * ny + y, x]
            )
            total += first_in1[pair, y, x].astype(f32)
        return total

    def reduce_own(core):
        owner = my_pair * 2 + core
        if core == 0:
            others = [(half_sum0, summed0, y, device_at(owner, y, my_x)) for y in others_y]
            arriving, sent, received, here = own_in0, own0_send, own0_recv, my_y
        else:
            others = [(half_sum1, summed1, x, device_at(owner, my_y, x)) for x in others_x]
            arriving, sent, received, here = own_in1, own1_send, own1_recv, my_x
        for sums, summed, place, target in others:
            sums[my_pair, place] = summed(my_pair, place).astype(bf16)
            start(
                sums.at[my_pair, place],
                arriving.at[my_core, here],
                sent.at[place],
                received.at[my_core, here],
                target,
            )

    def keep_own(core):
        mine = summed1(my_pair, my_x) if core else summed0(my_pair, my_y)
        own_part[core] = mine.astype(bf16)

        @pl.when(my_core != core)
        def _():
            copy_to(
                own_part.at[core],
                own_came,
                core_sem.at[0],
                core_sem.at[1],
                device_at(sibling, my_y, my_x),
            ).start()

    def finish_own():
        copy_to(
            own_came, own_came, core_sem.at[0], core_sem.at[1], device_at(me, my_y, my_x)
        ).wait_recv()
        for core in range(2):

            @pl.when(my_core == core)
            def _(core=core):
                arriving, received, sent, places = (
                    (own_in0, own0_recv, own0_send, others_y)
                    if core == 0
                    else (own_in1, own1_recv, own1_send, others_x)
                )
                for source in range(2):
                    part = own_part[core] if source == core else own_came[...]
                    total = part.astype(f32)
                    for place in places:
                        arrive(
                            arriving.at[source, place], sent.at[place], received.at[source, place]
                        )
                        total += arriving[source, place].astype(f32)
                    returned[slots_of(my_pair * 2 + source), :] = total.astype(bf16)

        copy_to(
            own_part.at[0], own_came, core_sem.at[0], core_sem.at[1], device_at(sibling, my_y, my_x)
        ).wait_send()

    def reduce_first(step, core):
        pair = pair_of[step]
        if step == 0:
            reduce_own(core)
        elif core == 0:
            for y in others_y:
                half_sum0[pair, y] = summed0(pair, y).astype(bf16)
                start(
                    half_sum0.at[pair, y],
                    second_in0.at[pair, my_y],
                    rb0_send.at[pair, y],
                    rb0_recv.at[pair, my_y],
                    device_at(me, y, my_x),
                )
        else:
            for x in others_x:
                half_sum1[pair, x] = summed1(pair, x).astype(bf16)
                start(
                    half_sum1.at[pair, x],
                    second_in1.at[pair, my_x],
                    rb1_send.at[pair, x],
                    rb1_recv.at[pair, my_x],
                    device_at(me, my_y, x),
                )

    def slots_of(expert):
        return pl.ds(pl.multiple_of(expert * slots, slots), slots)

    def give_back(target):
        start(
            finished.at[target],
            returned.at[slots_of(me)],
            back_send.at[target],
            back_recv.at[me],
            device_at(target, my_y, my_x),
        )

    def reduce_second(step, core):
        pair = pair_of[step]
        if step == 0:
            if core == 0:
                keep_own(0)
                keep_own(1)
            else:
                while pending:
                    pending.pop(0).wait_send()
                finish_own()
            return
        if core == 0:
            total = summed0(pair, my_y)
            for y in others_y:
                arrive(second_in0.at[pair, y], rb0_send.at[pair, y], rb0_recv.at[pair, y])
                total += second_in0[pair, y].astype(f32)
        else:
            total = summed1(pair, my_x)
            for x in others_x:
                arrive(second_in1.at[pair, x], rb1_send.at[pair, x], rb1_recv.at[pair, x])
                total += second_in1[pair, x].astype(f32)
        finished[pair * 2 + core] = total.astype(bf16)
        give_back(pair * 2 + core)

    actions = {
        "ZS": go_own,
        "ZD": go_far,
        "SB": go_sibling,
        "PS": pool_start,
        "PE": pool_end,
        "OWN": own_rows,
        "SF": spread_own,
        "SS": relay,
        "SE": spread_end,
        "GU": gate_up,
        "DN": down,
        "SP": send_parts,
        "RF": reduce_first,
        "R2": reduce_second,
    }
    for name, step, part in plan(pairs):
        actions[name](step, part)
    for step in range(1, pairs):
        for core in range(2):
            source = pair_of[step] * 2 + core
            arrive(returned.at[slots_of(source)], back_send.at[source], back_recv.at[source])
    out_ref[...] = jnp.dot(blend_ref[...], returned[...], preferred_element_type=f32).astype(bf16)
    for copy in pending:
        copy.wait_send()


def store_kernel(pool_ref, expert_ref, pool_hbm, expert_hbm, sems):
    copies = [
        pltpu.make_async_copy(source, target, sems.at[number])
        for number, (source, target) in enumerate(
            ((pool_ref, pool_hbm), (expert_ref, expert_hbm))
        )
    ]
    for copy in copies:
        copy.start()
    for copy in copies:
        copy.wait()


def local(
    pool_input,
    pool_gain,
    pool_weight,
    pool_scale,
    moe_input,
    moe_gain,
    routes,
    route_logits,
    gate_weight,
    up_weight,
    down_weight,
):
    local_rows, row_width = moe_input.shape
    picks_count = routes.shape[1]
    experts, shards = lax.axis_size("ep"), lax.axis_size("tp")
    capacity = 2 * local_rows * picks_count // experts
    slots = -(-capacity // 16) * 16
    columns = row_width // shards
    ny = max(d for d in range(1, shards + 1) if shards % d == 0 and d * d <= shards)
    nx = shards // ny
    pairs = experts // 2
    hidden_units = gate_weight.shape[2]
    pool_rows, group_width = pool_input.shape[0], pool_weight.shape[0]

    bf16, f32 = jnp.bfloat16, jnp.float32
    dma = pltpu.SemaphoreType.DMA
    vmem = pl.BlockSpec(memory_space=pltpu.VMEM)
    anywhere = pl.BlockSpec(memory_space=pl.ANY)
    block = (slots, columns)
    sems_x, sems_y = dma((pairs, nx)), dma((pairs, ny))
    spread_sems = dma((experts * ny, nx))
    far_count = (ny - 1) * (nx - 1)
    expert_out, pool_out = pl.pallas_call(
        functools.partial(expert_kernel, (experts, ny, nx, slots, columns)),
        out_shape=(
            pltpu.VMEM((local_rows, columns), bf16),
            pltpu.VMEM((pool_rows, pool_weight.shape[1]), bf16),
        ),
        in_specs=[anywhere] * 11,
        out_specs=(vmem, vmem),
        scratch_shapes=[
            pltpu.VMEM((picks_count, local_rows), jnp.int32),
            pltpu.VMEM((picks_count, local_rows), f32),
            pltpu.VMEM((1, row_width), f32),
            pltpu.VMEM((1, row_width), f32),
            pltpu.VMEM((1, pool_weight.shape[1]), f32),
            pltpu.VMEM((local_rows, row_width), bf16),
            pltpu.VMEM((pool_rows, row_width), bf16),
            pltpu.VMEM(pool_weight.shape, bf16),
            pltpu.VMEM((experts, local_rows), f32),
            pltpu.VMEM((local_rows, experts * slots), bf16),
            pltpu.VMEM((local_rows, row_width), bf16),
            pltpu.VMEM((experts,) + block, bf16),
            pltpu.VMEM((far_count, experts) + block, bf16),
            pltpu.VMEM((ny, nx) + block, bf16),
            pltpu.VMEM((pairs, ny, nx, 2 * slots, columns), bf16),
            pltpu.VMEM((pairs, 2 * slots, hidden_units), bf16),
            pltpu.VMEM((pairs, ny, nx, 2 * slots, columns), bf16),
            pltpu.VMEM((pairs, nx, ny) + block, bf16),
            pltpu.VMEM((pairs, ny, nx) + block, bf16),
            pltpu.VMEM((pairs, ny) + block, bf16),
            pltpu.VMEM((pairs, nx) + block, bf16),
            pltpu.VMEM((pairs, ny) + block, bf16),
            pltpu.VMEM((pairs, nx) + block, bf16),
            pltpu.VMEM((2, ny) + block, bf16),
            pltpu.VMEM((2, nx) + block, bf16),
            pltpu.VMEM((2,) + block, bf16),
            pltpu.VMEM(block, bf16),
            pltpu.VMEM((experts,) + block, bf16),
            pltpu.VMEM((experts * slots, columns), bf16),
            pltpu.VMEM((row_width, hidden_units), bf16),
            pltpu.VMEM((row_width, hidden_units), bf16),
            pltpu.VMEM((row_width, hidden_units), bf16),
            pltpu.VMEM((pool_rows, group_width), bf16),
            pltpu.VMEM((halo_rows, group_width), bf16),
            pltpu.VMEM((halo_rows, group_width), bf16),
            dma((11,)),
            dma((2,)),
            dma((experts,)),
            dma((experts,)),
        ]
        + [dma((far_count, experts)), spread_sems, spread_sems]
        + [dma((pairs * nx, ny))] * 2
        + [dma((pairs * ny, nx))] * 2
        + [sems_y, sems_y, sems_x, sems_x]
        + [dma((ny,)), dma((2, ny)), dma((nx,)), dma((2, nx)), dma((2,))]
        + [dma((experts,)), dma((experts,))],
        compiler_params=pltpu.CompilerParams(
            collective_id=0, has_side_effects=True, vmem_limit_bytes=56 * 1024 * 1024
        ),
    )(
        routes.T,
        route_logits.T,
        moe_gain.reshape(1, row_width),
        pool_gain.reshape(1, row_width),
        pool_scale.reshape(1, -1),
        moe_input,
        gate_weight,
        up_weight,
        down_weight,
        pool_input,
        pool_weight,
    )
    return pl.pallas_call(
        store_kernel,
        out_shape=(
            jax.ShapeDtypeStruct(pool_out.shape, bf16),
            jax.ShapeDtypeStruct(expert_out.shape, bf16),
        ),
        in_specs=[vmem, vmem],
        out_specs=(anywhere, anywhere),
        scratch_shapes=[dma((2,))],
        compiler_params=pltpu.CompilerParams(vmem_limit_bytes=1024 * 1024),
    )(pool_out, expert_out)


def solution(mesh):
    in_specs = (
        P("ep", None),
        P(),
        P(None, "tp"),
        P("tp"),
        P("ep", None),
        P(),
        P("ep", None),
        P("ep", None),
        P("ep", None, "tp"),
        P("ep", None, "tp"),
        P("ep", None, "tp"),
    )
    out_specs = (P("ep", "tp"), P("ep", "tp"))
    return jax.shard_map(local, mesh=mesh, in_specs=in_specs, out_specs=out_specs, check_vma=False)
```
